32 devices in a mesh: sp: 8 (over z, y), tp: 4 (over x, core).
Axes of the slice: x: 2, y: 2, z: 4, core: 2. Of those that a mesh axis runs over, the one named last changes fastest.
Arguments:
- tokens: bfloat16 [3072, 2048], P('sp'), may hold values from -6 to 6
- in_gain: float32 [2048], replicated, may hold values from 0.1 to 1.9
- query_weight: bfloat16 [2048, 1024], P(None, 'tp'), may hold values from -0.125 to 0.125
- key_weight: bfloat16 [2048, 1024], P(None, 'tp'), may hold values from -0.125 to 0.125
- value_weight: bfloat16 [2048, 2048], P(None, 'tp'), may hold values from -0.125 to 0.125
- gate_weight: bfloat16 [2048, 2048], P(None, 'tp'), may hold values from -0.125 to 0.125
- decay_down: bfloat16 [2048, 32], replicated, may hold values from -0.125 to 0.125
- decay_up: bfloat16 [32, 1024], replicated, may hold values from -1 to 1
- decay_offset: float32 [1024], P('tp')
- decay_extra: float32 [3072, 1024], P('sp', 'tp'), may hold values from -2 to 0, as said below
- head_gain: float32 [2048], P('tp'), may hold values from 0.1 to 1.9
- out_weight: bfloat16 [2048, 2048], P(None, 'tp'), may hold values from -4 to 4
- out_gain: float32 [2048], P('tp'), may hold values from 0.1 to 1.9
Outputs:
- layer_output: bfloat16 [3072, 2048], P('sp', 'tp')
The draws below stay inside these ranges and needn't reach their ends.
Inputs may be any that keep to these rules, and one draw needn't show every extreme that they name: `decay_extra`: never positive.
All inputs are finite; a program needn't handle non-finite values.
Results may differ from the reference program's by a relative error of at most 0.015.
Values may be sent and summed in bfloat16 or wider, within the bound.
A program may use at most 64 MiB of HBM per device.

```python
import math
import jax
import jax.numpy as jnp
from jax import lax

D = 2048
ATTENTION_UNITS = 8
QUERY_FEATURES = 128
DV = 256
RANK = 32
BLOCK = 64
TOK = 384
TOKEN_SPAN = 3072
KW = 1024
VW = 2048


def draw_decay_offset(key, part):
    base_key = jax.random.fold_in(key, 11)
    order_key, jitter_key = jax.random.split(base_key)
    jitter = jax.random.uniform(jitter_key, (ATTENTION_UNITS, QUERY_FEATURES), jnp.float32, -0.5, 0.5)
    slow_level = math.log(4.0 * TOKEN_SPAN / 16.0)
    ranking = jax.random.permutation(order_key, ATTENTION_UNITS)
    slow_heads = (ranking < ATTENTION_UNITS // 2)[:, None]
    levels = jnp.where(slow_heads, slow_level, 0.0) + jitter
    return levels.reshape(ATTENTION_UNITS * QUERY_FEATURES).astype(jnp.float32)


def draw_decay_extra(key, part):
    base_key = jax.random.fold_in(key, 23)
    rate_key, channel_key, place_key, depth_key = jax.random.split(base_key, 4)
    block_total = TOKEN_SPAN // TOK
    block_rates = jnp.exp(jax.random.uniform(rate_key, (block_total, 1, ATTENTION_UNITS, 1), jnp.float32, math.log(0.1), math.log(2.0)))
    channel_rates = jnp.exp(jax.random.uniform(channel_key, (1, 1, ATTENTION_UNITS, QUERY_FEATURES), jnp.float32, math.log(0.5), math.log(2.0)))
    constant_amount = jnp.broadcast_to(-(block_rates * channel_rates) / TOKEN_SPAN, (block_total, TOK, ATTENTION_UNITS, QUERY_FEATURES))
    location_cells = jax.random.randint(place_key, (2, ATTENTION_UNITS), 0, TOKEN_SPAN)
    layer_tiers = jax.random.uniform(depth_key, (2, ATTENTION_UNITS), jnp.float32, math.log(0.5), math.log(0.8))
    token_ordinal = jnp.arange(TOKEN_SPAN)[:, None, None]
    packet_clusters = jnp.sum(jnp.where(token_ordinal == location_cells[None], layer_tiers[None], 0.0), axis=1)
    overall_number = constant_amount.reshape(TOKEN_SPAN, ATTENTION_UNITS, QUERY_FEATURES) + packet_clusters[:, :, None]
    return overall_number.reshape(TOKEN_SPAN, ATTENTION_UNITS * QUERY_FEATURES).astype(jnp.float32)


def draw_out_weight(key, part):
    base_key = jax.random.fold_in(key, 37)
    weight_key, jitter_key = jax.random.split(base_key)
    values = jax.random.truncated_normal(weight_key, -4.0, 4.0, (VW, D), jnp.float32) / math.sqrt(VW)
    columns = jnp.arange(D).astype(jnp.float32) / D
    jitter = jax.random.uniform(jitter_key, (D,), jnp.float32, 0.0, 1.0)
    exponent = (columns + jitter / 8.0) / 1.125
    return (values * jnp.power(10.0, exponent)[None, :]).astype(jnp.bfloat16)


def steps_of(rng, extent, shards, smallest, largest):
    loudness, own = 1.0, jax.random.fold_in(rng, 6)
    for dim, shards_of in shards:
        draws = jnp.exp(jax.random.uniform(jax.random.fold_in(own, dim), (shards_of,), jnp.float32, smallest / len(shards), largest / len(shards)))
        loudness = loudness * jnp.repeat(draws, extent[dim] // shards_of).reshape([-1 if axis == dim else 1 for axis in range(len(extent))])
    return loudness


def bell_draw(rng, extent, spread, most, shards=(), dtype=jnp.bfloat16):
    factor_of = steps_of(rng, extent, shards, -0.22, 0.18) if shards else 1.0
    array = jax.random.normal(rng, extent, jnp.float32) * spread * factor_of
    return jnp.minimum(jnp.maximum(array, -most), most).astype(dtype)


def setup_inputs(seed: int = 0) -> dict:
    key_of = jax.random.split(jax.random.key(seed), 14)
    return {
        "tokens": bell_draw(key_of[0], (TOKEN_SPAN, D), 1.0, 6.0, ((0, 8),)),
        "in_gain": jnp.clip(1.0 + 0.18 * jax.random.normal(key_of[1], (D,), jnp.float32), 0.1, 1.9),
        "query_weight": bell_draw(key_of[2], (D, KW), D ** -0.5, 0.125, ((1, 4),)),
        "key_weight": bell_draw(key_of[3], (D, KW), D ** -0.5, 0.125, ((1, 4),)),
        "value_weight": bell_draw(key_of[4], (D, VW), D ** -0.5, 0.125, ((1, 4),)),
        "gate_weight": bell_draw(key_of[5], (D, VW), D ** -0.5, 0.125, ((1, 4),)),
        "decay_down": bell_draw(key_of[6], (D, RANK), D ** -0.5, 0.125),
        "decay_up": bell_draw(key_of[7], (RANK, KW), RANK ** -0.5, 1.0),
        "decay_offset": draw_decay_offset(jax.random.fold_in(key_of[13], 71), 0),
        "decay_extra": draw_decay_extra(jax.random.fold_in(key_of[13], 71), 0),
        "head_gain": jnp.clip(1.0 + 0.18 * jax.random.normal(key_of[10], (VW,), jnp.float32), 0.1, 1.9),
        "out_weight": draw_out_weight(jax.random.fold_in(key_of[13], 71), 0),
        "out_gain": jnp.clip(1.0 + 0.18 * jax.random.normal(key_of[12], (D,), jnp.float32), 0.1, 1.9),
    }


norm_eps = 1e-06
decay_temper = 16.0

def reference(tokens, in_gain, query_weight, key_weight, value_weight, gate_weight, decay_down, decay_up, decay_offset, decay_extra, head_gain, out_weight, out_gain):
    highest = lax.Precision.HIGHEST
    tokens_wide = tokens.astype(jnp.float32)
    normed = (tokens_wide * lax.rsqrt(lax.optimization_barrier(jnp.mean(tokens_wide * tokens_wide, axis=1, keepdims=True)) + norm_eps) * in_gain).astype(jnp.bfloat16)

    def project(weight):
        return jnp.dot(normed, weight, preferred_element_type=jnp.float32).astype(jnp.bfloat16)
    query_rows = project(query_weight)
    key_rows = project(key_weight)
    value_rows = project(value_weight)
    gate_rows = project(gate_weight)
    low_rank = project(decay_down)
    logits = jnp.dot(low_rank, decay_up, preferred_element_type=jnp.float32)
    log_decay = jax.nn.log_sigmoid(logits + decay_offset) / decay_temper + decay_extra
    block_count = TOKEN_SPAN // BLOCK

    def to_blocks(values, width):
        return values.astype(jnp.float32).reshape(block_count, BLOCK, ATTENTION_UNITS, width)
    causal_mask = jnp.arange(BLOCK)[:, None] >= jnp.arange(BLOCK)[None, :]

    def block_step(carry_state, inputs):
        query_block, key_block, value_block, decay_block = inputs
        cumulative = jnp.cumsum(decay_block, axis=0)
        closing = cumulative[-1]
        query_inner = query_block * jnp.exp(cumulative)
        key_inner = key_block * jnp.exp(-cumulative)
        scores = jnp.einsum('chd,shd->hcs', query_inner, key_inner, precision=highest)
        scores = jnp.where(causal_mask[None], scores, 0.0)
        output = jnp.einsum('hcs,she->che', scores, value_block, precision=highest)
        output = output + jnp.einsum('chd,hde->che', query_inner, carry_state, precision=highest)
        key_closing = key_block * jnp.exp(closing[None] - cumulative)
        carry_state = carry_state * jnp.exp(closing)[:, :, None] + jnp.einsum('chd,che->hde', key_closing, value_block, precision=highest)
        return (carry_state, output)
    start_state = jnp.zeros((ATTENTION_UNITS, QUERY_FEATURES, DV), jnp.float32)
    final_state, outputs = lax.scan(block_step, start_state, (to_blocks(query_rows, QUERY_FEATURES), to_blocks(key_rows, QUERY_FEATURES), to_blocks(value_rows, DV), to_blocks(log_decay, QUERY_FEATURES)))
    attended = outputs.reshape(TOKEN_SPAN, ATTENTION_UNITS, DV)
    scaled = attended * lax.rsqrt(lax.optimization_barrier(jnp.mean(attended * attended, axis=2, keepdims=True)) + norm_eps) * head_gain.reshape(ATTENTION_UNITS, DV)
    gated = (scaled.reshape(TOKEN_SPAN, ATTENTION_UNITS * DV) * jax.nn.silu(gate_rows.astype(jnp.float32))).astype(jnp.bfloat16)
    mixed = jnp.dot(gated, out_weight, preferred_element_type=jnp.float32)
    result = mixed * lax.rsqrt(lax.optimization_barrier(jnp.mean(mixed * mixed, axis=1, keepdims=True)) + norm_eps) * out_gain
    return result.astype(jnp.bfloat16)
```

```python
import functools

import jax
import jax.numpy as jnp
from jax import lax
from jax.experimental import pallas as pl
from jax.experimental.pallas import tpu as pltpu
from jax.sharding import PartitionSpec as P

QF = 128
DV = 256
BLK = 128
HALF = 64
TOK_CHUNKS = 4
EPS = 1e-06
F32 = jnp.float32
BF16 = jnp.bfloat16
MESH = pl.DeviceIdType.MESH


def loop(count, body, carry):
    if count <= 16:
        for i in range(count):
            carry = body(i, carry)
        return carry
    return lax.fori_loop(0, count, body, carry)


def split3(x):
    hi = x.astype(BF16)
    rest = x - hi.astype(F32)
    mid = rest.astype(BF16)
    lo = (rest - mid.astype(F32)).astype(BF16)
    return hi, mid, lo


def dot(a, b):
    return jnp.dot(a, b, preferred_element_type=F32)


def dot_nt(a, b):
    return lax.dot_general(a, b, (((1,), (1,)), ((), ())), preferred_element_type=F32)


def dot_tn(a, b):
    return lax.dot_general(a, b, (((0,), (0,)), ((), ())), preferred_element_type=F32)


def kernel(
    n, n_tp, owners, piece, start,
    tok_hbm, in_gain_hbm, wq_hbm, wk_hbm, wv_hbm, wg_hbm, down_hbm, up_hbm, offset_hbm,
    extra_hbm, head_gain_hbm, wo_hbm, out_gain_hbm,
    out,
    tok, wq, wk, wv, wg, down, up, extra, wo, in_gain, offset, head_gain, out_gain,
    nrm, q_s, k_s, v_s, g_s, cum_s, att, qd_s, before, mix,
    send1, recv1, send2, recv2, logs, gath, sq,
    tok_sem, load_sem, sl_sem, rl_sem, s1_sem, r1_sem, s2_sem, r2_sem,
    gs_sem, gr_sem, qs_sem, qr_sem,
):
    rows, width = tok.shape
    chans = wk.shape[1]
    heads = chans // QF
    vals = wv.shape[1]
    blocks = rows // BLK
    me = lax.axis_index("sp")
    tp = lax.axis_index("tp")
    chips = n_tp // 2
    core = lax.rem(tp, 2)
    chip = tp // 2
    partner = chip * 2 + (1 - core)
    own = me - start
    owning = jnp.logical_and(own >= 0, own < owners)

    first = pl.multiple_of(tp * chans, chans)
    chunk = rows // TOK_CHUNKS
    tok_load = [
        pltpu.make_async_copy(
            tok_hbm.at[pl.ds(i * chunk, chunk)], tok.at[pl.ds(i * chunk, chunk)], tok_sem.at[i]
        )
        for i in range(TOK_CHUNKS)
    ]
    load = {
        name: pltpu.make_async_copy(src, dst, load_sem.at[i])
        for i, (name, src, dst) in enumerate(
            (
                ("in_gain", in_gain_hbm, in_gain),
                ("wk", wk_hbm, wk),
                ("down", down_hbm, down),
                ("up", up_hbm.at[:, pl.ds(first, chans)], up),
                ("extra", extra_hbm, extra),
                ("offset", offset_hbm, offset),
                ("wv", wv_hbm, wv),
                ("wq", wq_hbm, wq),
                ("wg", wg_hbm, wg),
                ("head_gain", head_gain_hbm, head_gain),
                ("wo", wo_hbm, wo),
                ("out_gain", out_gain_hbm, out_gain),
            )
        )
    }

    def begin(*names):
        for name in names:
            load[name].start()

    def arrive(*names):
        for name in names:
            load[name].wait()

    begin("in_gain")
    for one in tok_load:
        one.start()
    begin("down", "wk", "up", "offset", "extra")

    barrier = pltpu.get_barrier_semaphore()

    def greet_sp(d, carry):
        pl.semaphore_signal(
            barrier, inc=1, device_id={"sp": lax.rem(me + d + 1, n)}, device_id_type=MESH
        )
        return carry

    loop(n - 1, greet_sp, 0)
    for d in range(1, n_tp):
        pl.semaphore_signal(
            barrier, inc=1, device_id={"tp": lax.rem(tp + d, n_tp)}, device_id_type=MESH
        )

    step = 32
    arrive("in_gain")
    for i in range(TOK_CHUNKS):
        tok_load[i].wait()
        if i == TOK_CHUNKS - 2:
            begin("wv")

        def norm_rows(j, carry):
            where = pl.ds(pl.multiple_of(i * chunk + j * step, step), step)
            wide = tok[where, :].astype(F32)
            scale = lax.rsqrt(jnp.sum(wide * wide, axis=1, keepdims=True) * (1.0 / width) + EPS)
            nrm[where, :] = (wide * scale * in_gain[...]).astype(BF16)
            return carry

        lax.fori_loop(0, chunk // step, norm_rows, 0, unroll=True)

    arrive("down", "wk")
    begin("wq", "wg", "head_gain", "wo", "out_gain")
    low = dot_nt(nrm[...], down[...]).astype(BF16)
    k_s[...] = dot(nrm[...], wk[...]).astype(BF16)
    arrive("up", "offset", "extra", "wv")
    logits = dot(low, up[...]) + offset[...]
    log_sig = jnp.minimum(logits, 0.0) - jnp.log1p(jnp.exp(-jnp.abs(logits)))
    decay = log_sig * (1.0 / 16.0) + extra[...]
    tri = (
        lax.broadcasted_iota(jnp.int32, (BLK, BLK), 0)
        >= lax.broadcasted_iota(jnp.int32, (BLK, BLK), 1)
    )
    tri_ones = tri.astype(F32).astype(BF16)
    for h in range(heads):
        cols = slice(h * DV, (h + 1) * DV)
        v_s[:, cols] = dot(nrm[...], wv[:, cols]).astype(BF16)
    for b in range(blocks):
        hi, mid, lo = split3(decay[b * BLK:(b + 1) * BLK, :])
        cum_s[b * BLK:(b + 1) * BLK, :] = (
            dot(tri_ones, hi) + dot(tri_ones, mid) + dot(tri_ones, lo)
        )
    totals = [cum_s[b * BLK + BLK - 1:(b + 1) * BLK, :] for b in range(blocks)]
    device_log = totals[0]
    for one in totals[1:]:
        device_log = device_log + one
    logs[me] = device_log

    def log_to_owner(p):
        return pltpu.make_async_remote_copy(
            src_ref=logs.at[me], dst_ref=logs.at[me], send_sem=sl_sem, recv_sem=rl_sem,
            device_id={"sp": start + p}, device_id_type=MESH,
        )

    def to_owner(h, p):
        return pltpu.make_async_remote_copy(
            src_ref=send1.at[h, p], dst_ref=recv1.at[h, me],
            send_sem=s1_sem, recv_sem=r1_sem.at[h, me],
            device_id={"sp": start + p}, device_id_type=MESH,
        )

    def from_source(h, i):
        return pltpu.make_async_remote_copy(
            src_ref=send1.at[h, 0], dst_ref=recv1.at[h, i],
            send_sem=s1_sem, recv_sem=r1_sem.at[h, i],
            device_id={"sp": i}, device_id_type=MESH,
        )

    def to_user(h, i):
        return pltpu.make_async_remote_copy(
            src_ref=send2.at[h, i], dst_ref=recv2.at[h, own],
            send_sem=s2_sem, recv_sem=r2_sem.at[h],
            device_id={"sp": i}, device_id_type=MESH,
        )

    def settle(ref, sem):
        pltpu.make_async_copy(ref, ref, sem).wait()

    def each_owner(action):
        @pl.when(me < n - 1)
        def _():
            def one(d, carry):
                p = lax.rem(me + d, owners)

                @pl.when(start + p != me)
                def _():
                    action(p)

                return carry

            loop(owners, one, 0)

    pl.semaphore_wait(barrier, n - 1 + n_tp - 1)
    each_owner(lambda p: log_to_owner(p).start())

    for h in range(heads):
        ch = slice(h * QF, (h + 1) * QF)
        cols = slice(h * DV, (h + 1) * DV)
        for b in range(blocks):
            part = slice(b * BLK, (b + 1) * BLK)
            total = totals[b][:, ch]
            closing = (k_s[part, ch].astype(F32) * jnp.exp(total - cum_s[part, ch])).astype(BF16)
            fresh = dot_tn(v_s[part, cols], closing)
            if b:
                fresh = fresh + before[b - 1, :, ch] * jnp.exp(total)
            before[b, :, ch] = fresh
        for p in range(owners):
            send1[h, p] = before[blocks - 1, p * piece:(p + 1) * piece, ch].astype(BF16)
        each_owner(lambda p: to_owner(h, p).start())

    arrive("wq", "wg", "head_gain")
    for c in range(0, chans, 256):
        cols = slice(c, min(c + 256, chans))
        q_s[:, cols] = dot(nrm[...], wq[:, cols]).astype(BF16)
    for c in range(vals // DV):
        cols = slice(c * DV, (c + 1) * DV)
        gate = dot(nrm[...], wg[:, cols]).astype(BF16).astype(F32)
        g_s[:, cols] = gate * jax.nn.sigmoid(gate) * head_gain[:, cols]

    device_log = jnp.zeros((1, chans), F32)
    for b in range(blocks):
        part = slice(b * BLK, (b + 1) * BLK)
        cum = cum_s[part, :]
        total = cum[BLK - 1:BLK, :]
        middle = cum[HALF - 1:HALF, :]
        query = q_s[part, :].astype(F32)
        key = k_s[part, :].astype(F32)
        query_inner = (query * jnp.exp(cum - middle)).astype(BF16)
        key_inner = (key * jnp.exp(middle - cum)).astype(BF16)
        qd_s[part, :] = (query * jnp.exp(cum + device_log)).astype(BF16)
        query_start = (query * jnp.exp(cum)).astype(BF16)
        for h in range(heads):
            ch = slice(h * QF, (h + 1) * QF)
            scores = dot_nt(query_inner[:, ch], key_inner[:, ch])
            scores = jnp.where(tri, scores, 0.0).astype(BF16)
            result = dot(scores, v_s[part, h * DV:(h + 1) * DV])
            if b:
                result = result + dot_nt(query_start[:, ch], before[b - 1, :, ch].astype(BF16))
            att[part, h * DV:(h + 1) * DV] = result
        device_log = device_log + total

    def prefixes(h):
        recv1[h, me] = send1[h, own]

        def one(i, state):
            rounded = state.astype(BF16)

            @pl.when(i == me)
            def _():
                recv2[h, own] = rounded

            @pl.when(jnp.logical_and(i != me, i > 0))
            def _():
                send2[h, i] = rounded
                to_user(h, i).start()

            @pl.when(jnp.logical_and(i != me, i < n - 1))
            def _():
                from_source(h, i).wait_recv()

            last = jnp.minimum(i, n - 2)
            log = logs[last][:, h * QF:(h + 1) * QF]
            return state * jnp.exp(log) + recv1[h, last].astype(F32)

        loop(n, one, jnp.zeros((piece, QF), F32))

    @pl.when(owning)
    def _():
        settle(logs.at[pl.ds(0, n - 2)], rl_sem)
        for h in range(heads):
            prefixes(h)

    def gather_copy(slot, h, b, to, which):
        part = pl.ds(b * BLK, BLK)
        return pltpu.make_async_remote_copy(
            src_ref=gath.at[slot, h, part], dst_ref=gath.at[slot, h, part],
            send_sem=gs_sem, recv_sem=gr_sem.at[which, h, b],
            device_id={"tp": to}, device_id_type=MESH,
        )

    def chip_at(d):
        return lax.rem(chip + d + chips, chips)

    @pl.when(me == 0)
    def _():
        recv2[...] = jnp.zeros_like(recv2)

    for h in range(heads):
        ch = slice(h * QF, (h + 1) * QF)
        cols = slice(h * DV, (h + 1) * DV)

        @pl.when(owning)
        def _():
            settle(recv2.at[h, pl.ds(0, owners - 1)], r2_sem.at[h])

        @pl.when(jnp.logical_and(me > 0, jnp.logical_not(owning)))
        def _():
            settle(recv2.at[h], r2_sem.at[h])

        carried = jnp.concatenate([recv2[h, p] for p in range(owners)], axis=0)
        for b in range(blocks):
            part = slice(b * BLK, (b + 1) * BLK)
            full = att[part, cols] + dot_nt(qd_s[part, ch], carried)
            scale = lax.rsqrt(jnp.mean(full * full, axis=1, keepdims=True) + EPS)
            gath[tp, h, part, :] = (full * scale * g_s[part, cols]).astype(BF16)
            for d in range(1, chips):
                gather_copy(tp, h, b, chip_at(d) * 2 + core, d).start()
            gather_copy(tp, h, b, partner, 0).start()

    arrive("wo", "out_gain")

    def add(slot, h, part, begin):
        first = pl.multiple_of(slot * vals + h * DV, DV)
        value = dot(gath[slot, h, part, :], wo[pl.ds(first, DV), :])
        if begin:
            mix[part, :] = value
        else:
            mix[part, :] += value

    whole = slice(0, rows)
    for h in range(heads):
        add(tp, h, whole, h == 0)
    for h in range(heads):
        for b in range(blocks):
            gather_copy(partner, h, b, partner, 0).wait_recv()
        add(partner, h, whole, False)
    for h in range(heads):
        for d in range(1, chips):
            slot = chip_at(-d) * 2 + core
            for b in range(blocks):
                gather_copy(slot, h, b, partner, d).wait_recv()
                gather_copy(slot, h, b, partner, chips - 1 + d).start()
                if h == heads - 1:
                    add(slot, h, slice(b * BLK, (b + 1) * BLK), False)
            if h < heads - 1:
                add(slot, h, whole, False)
        for d in range(1, chips):
            slot = chip_at(-d) * 2 + (1 - core)
            if h < heads - 1:
                for b in range(blocks):
                    gather_copy(slot, h, b, partner, chips - 1 + d).wait_recv()
                add(slot, h, whole, False)
    def square_copy(d, b):
        return pltpu.make_async_remote_copy(
            src_ref=sq.at[0, b], dst_ref=sq.at[d, b],
            send_sem=qs_sem, recv_sem=qr_sem.at[b],
            device_id={"tp": lax.rem(tp + d, n_tp)}, device_id_type=MESH,
        )

    lanes = 128
    feats = wo.shape[1]
    for b in range(blocks):
        part = slice(b * BLK, (b + 1) * BLK)
        for d in range(1, chips):
            slot = chip_at(-d) * 2 + (1 - core)
            gather_copy(slot, heads - 1, b, partner, chips - 1 + d).wait_recv()
            add(slot, heads - 1, part, False)
        squares = jnp.zeros((BLK, lanes), F32)
        for c in range(0, feats, lanes):
            value = mix[part, c:c + lanes]
            squares = squares + value * value
        row = jnp.sum(squares.T, axis=0, keepdims=True)
        sq[0, b] = jnp.broadcast_to(row, (8, BLK))
        for d in range(1, n_tp):
            square_copy(d, b).start()

    for b in range(blocks):
        part = slice(b * BLK, (b + 1) * BLK)
        settle(sq.at[pl.ds(1, n_tp - 1), b], qr_sem.at[b])
        total = sq[0, b]
        for d in range(1, n_tp):
            total = total + sq[d, b]
        row = jnp.broadcast_to(total[0:1, :], (lanes, BLK))
        scale = lax.rsqrt(row.T * (1.0 / width) + EPS)
        for c in range(0, feats, lanes):
            cols = slice(c, c + lanes)
            out[part, cols] = (mix[part, cols] * scale * out_gain[:, cols]).astype(BF16)

    @pl.when(owning)
    def _():
        settle(logs.at[pl.ds(0, owners - 1)], sl_sem)
        settle(send1.at[:, pl.ds(0, owners - 1)], s1_sem)
        settle(send2.at[:, pl.ds(0, n - 2)], s2_sem)

    @pl.when(jnp.logical_and(me < n - 1, jnp.logical_not(owning)))
    def _():
        settle(logs.at[pl.ds(0, owners)], sl_sem)
        settle(send1, s1_sem)

    settle(gath.at[pl.ds(0, n_tp - 1)], gs_sem)
    settle(sq.at[pl.ds(1, n_tp - 1)], qs_sem)


def local(n, n_tp, *args):
    (tokens, in_gain, wq, wk, wv, wg, down, up, offset, extra, head_gain, wo, out_gain) = args
    rows, width = tokens.shape
    chans, vals, feats = wk.shape[1], wv.shape[1], wo.shape[1]
    blocks = rows // BLK
    piece = max(16, 2 * DV // n)
    owners = DV // piece
    start = (n - owners) // 2
    heads = chans // QF
    hbm = pl.BlockSpec(memory_space=pltpu.HBM)
    dma = pltpu.SemaphoreType.DMA
    return pl.pallas_call(
        functools.partial(kernel, n, n_tp, owners, piece, start),
        out_shape=pltpu.VMEM((rows, feats), BF16),
        in_specs=[hbm] * 13,
        out_specs=pl.BlockSpec(memory_space=pltpu.VMEM),
        scratch_shapes=[
            pltpu.VMEM(tokens.shape, BF16),
            pltpu.VMEM(wq.shape, BF16),
            pltpu.VMEM(wk.shape, BF16),
            pltpu.VMEM(wv.shape, BF16),
            pltpu.VMEM(wg.shape, BF16),
            pltpu.VMEM(down.shape[::-1], BF16),
            pltpu.VMEM((down.shape[1], chans), BF16),
            pltpu.VMEM(extra.shape, F32),
            pltpu.VMEM(wo.shape, BF16),
            pltpu.VMEM((1, width), F32),
            pltpu.VMEM((1, chans), F32),
            pltpu.VMEM((1, vals), F32),
            pltpu.VMEM((1, feats), F32),
            pltpu.VMEM((rows, width), BF16),
            pltpu.VMEM((rows, chans), BF16),
            pltpu.VMEM((rows, chans), BF16),
            pltpu.VMEM((rows, vals), BF16),
            pltpu.VMEM((rows, vals), F32),
            pltpu.VMEM((rows, chans), F32),
            pltpu.VMEM((rows, vals), F32),
            pltpu.VMEM((rows, chans), BF16),
            pltpu.VMEM((blocks, DV, chans), F32),
            pltpu.VMEM((rows, feats), F32),
            pltpu.VMEM((heads, owners, piece, QF), BF16),
            pltpu.VMEM((heads, n, piece, QF), BF16),
            pltpu.VMEM((heads, n, piece, QF), BF16),
            pltpu.VMEM((heads, owners, piece, QF), BF16),
            pltpu.VMEM((n, 1, chans), F32),
            pltpu.VMEM((n_tp, heads, rows, DV), BF16),
            pltpu.VMEM((n_tp, blocks, 8, BLK), F32),
            dma((TOK_CHUNKS,)),
            dma((12,)),
            dma,
            dma,
            dma,
            dma((heads, n)),
            dma,
            dma((heads,)),
            dma,
            dma((n_tp - 1, heads, blocks)),
            dma,
            dma((blocks,)),
        ],
        compiler_params=pltpu.CompilerParams(
            collective_id=0, has_side_effects=True, vmem_limit_bytes=66000000
        ),
    )(
        tokens, in_gain[None], wq, wk, wv, wg, down.T, up, offset[None], extra,
        head_gain[None], wo, out_gain[None],
    )


def solution(mesh):
    placed = (
        P("sp", None),
        P(),
        P(None, "tp"),
        P(None, "tp"),
        P(None, "tp"),
        P(None, "tp"),
        P(),
        P(),
        P("tp"),
        P("sp", "tp"),
        P("tp"),
        P(None, "tp"),
        P("tp"),
    )
    return jax.shard_map(
        functools.partial(local, mesh.shape["sp"], mesh.shape["tp"]),
        mesh=mesh, in_specs=placed, out_specs=P("sp", "tp"), check_vma=False,
    )
```
